32 devices in a mesh: kv: 8 (over z, x), tp: 4 (over y, core).
Axes of the slice: x: 2, y: 2, z: 4, core: 2. Of those that a mesh axis runs over, the one named last changes fastest.
Arguments:
- layer_input: bfloat16 [256, 4096], P('tp', 'kv'), may hold values from -6 to 6
- seq_lengths: int32 [64], P('kv'), may hold values from 1 to 4, 112 in all
- delta_state: float32 [64, 16, 128, 128], P('kv', 'tp'), may hold values from -0.4 to 0.4
- attn_gain: bfloat16 [4096], replicated, may hold values from 0.099609375 to 1.8984375
- w_query: bfloat16 [4096, 2048], P('kv', 'tp'), may hold values from -0.09375 to 0.09375
- w_key: bfloat16 [4096, 2048], P('kv', 'tp'), may hold values from -0.09375 to 0.09375
- w_value: bfloat16 [4096, 2048], P('kv', 'tp'), may hold values from -0.09375 to 0.09375
- w_outgate: bfloat16 [4096, 2048], P('kv', 'tp'), may hold values from -0.09375 to 0.09375
- w_write: bfloat16 [4096, 16], P('kv', 'tp'), may hold values from -0.09375 to 0.09375
- w_forget: bfloat16 [4096, 16], P('kv', 'tp'), may hold values from -0.09375 to 0.09375
- forget_rate: float32 [16], P('tp'), may hold values from 0.02 to 2
- head_gain: float32 [128], replicated, may hold values from 0.1 to 1.9
- w_out: bfloat16 [2048, 4096], P('tp', 'kv'), may hold values from -0.125 to 0.125
- mixer_gain: bfloat16 [4096], replicated, may hold values from 0.099609375 to 1.8984375
- w_gate: bfloat16 [4096, 11264], P('kv', 'tp'), may hold values from -0.09375 to 0.09375
- w_up: bfloat16 [4096, 11264], P('kv', 'tp'), may hold values from -0.09375 to 0.09375
- w_down: bfloat16 [11264, 4096], P('tp', 'kv'), may hold values from -0.0546875 to 0.0546875
Outputs:
- layer_output: bfloat16 [256, 4096], P('tp', 'kv')
- next_state: float32 [64, 16, 128, 128], P('kv', 'tp')
The draws below stay inside these ranges and needn't reach their ends.
Inputs may be any that keep to these rules, and one draw needn't show every extreme that they name: `seq_lengths`: the lengths add up to 112.
All inputs are finite; a program needn't handle non-finite values. No bound on the sum of `seq_lengths` on one device may be relied on, other than what follows from the above.
Results may differ from the reference program's by a relative error of at most 0.024.
Values may be sent and summed in bfloat16 or wider, within the bound.
A program may use at most 64 MiB of HBM per device.

```python
import math
import jax
import jax.numpy as jnp
import numpy as np
from jax import lax

D = 4096
H = 16
DK = 128
FF = 11264
NEW = 4
SEQS = 64
ROWS = 256
HW = 2048
N_TP = 4


def steps_of(stream_key, dims, split, low, largest):
    def one(axis_at, blocks):
        steps = jax.random.uniform(jax.random.fold_in(jax.random.fold_in(stream_key, 6), axis_at), (blocks,), jnp.float32, low / len(split), largest / len(split))
        return jnp.repeat(jnp.exp(steps), dims[axis_at] // blocks).reshape((-1,) + (1,) * (len(dims) - axis_at - 1))

    loudness = one(*split[0])
    for cut in split[1:]:
        loudness = loudness * one(*cut)
    return loudness


def length_profile(count, total, bound, slope):
    weights = [(1 << 20) // math.isqrt(rank ** slope) + 1 for rank in range(2, count + 1)]
    surplus, counts = total - bound - (count - 1), [1] * (count - 1)
    while surplus > 0:
        candidates = [i for i in range(count - 1) if counts[i] < bound]
        whole, remaining = sum([weights[i] for i in candidates]), surplus
        for i in candidates:
            extra = min(bound - counts[i], max(1, remaining * weights[i] // whole), surplus)
            counts[i] = counts[i] + extra
            surplus = surplus - extra
    return np.array([bound] + counts)


def ragged(rng, amount, total, bound, lean):
    if amount == 2:
        one = jax.random.randint(rng, (), max(1, total - bound), min(bound, total - 1) + 1)
        return jnp.stack([one, total - one])
    sizes = jnp.asarray(length_profile(amount, total, bound, lean), jnp.int32)
    twos = (amount - 1) // 2
    source_of, taker = sizes[1:1 + 2 * twos:2], sizes[2:2 + 2 * twos:2]
    room = jnp.minimum(source_of - 1, bound - taker)
    moved = jax.random.randint(jax.random.fold_in(rng, 1), (twos,), 0, 1 << 20) % (room + 1)
    sizes = sizes.at[1:1 + 2 * twos:2].set(source_of - moved).at[2:2 + 2 * twos:2].set(taker + moved)
    return sizes[jax.random.permutation(jax.random.fold_in(rng, 2), amount)]


def bell_draw(rng, extent, spread, most, pieces=(), held_as=jnp.bfloat16):
    level = steps_of(rng, extent, pieces, -0.22, 0.18) if pieces else 1.0
    array = jax.random.normal(rng, extent, jnp.float32) * spread * level
    return jnp.minimum(jnp.maximum(array, -most), most).astype(held_as)


def setup_inputs(seed: int = 0) -> dict:
    key_of = jax.random.split(jax.random.key(seed), 18)
    layer_input = bell_draw(key_of[0], (ROWS, D), 1.0, 6.0, ((0, 4), (1, 8)))
    seq_lengths = ragged(key_of[1], SEQS, SEQS + 3 * SEQS // 4, NEW, 2).astype(jnp.int32)
    delta_state = bell_draw(key_of[2], (SEQS, H, DK, DK), 0.05, 0.4, ((0, 8), (1, 4)), jnp.float32)
    attn_gain = jnp.clip(1.0 + 0.18 * jax.random.normal(key_of[3], (D,), jnp.float32), 0.099609375, 1.8984375).astype(jnp.bfloat16)
    w_query = bell_draw(key_of[4], (D, HW), D ** -0.5, 0.09375, ((0, 8), (1, 4)))
    w_key = bell_draw(key_of[5], (D, HW), D ** -0.5, 0.09375, ((0, 8), (1, 4)))
    w_value = bell_draw(key_of[6], (D, HW), D ** -0.5, 0.09375, ((0, 8), (1, 4)))
    w_outgate = bell_draw(key_of[7], (D, HW), D ** -0.5, 0.09375, ((0, 8), (1, 4)))
    w_write = bell_draw(key_of[8], (D, H), D ** -0.5, 0.09375, ((0, 8), (1, 4)))
    w_forget = bell_draw(key_of[9], (D, H), D ** -0.5, 0.09375, ((0, 8), (1, 4)))
    forget_rate = jnp.clip(jnp.exp(math.log(2.0) - 4.6051702 * jax.random.uniform(key_of[10], (H,), jnp.float32) ** steps_of(key_of[10], (H,), ((0, 4),), -0.2, 0.2)), 0.02, 2.0)
    head_gain = jnp.clip(1.0 + 0.18 * jax.random.normal(key_of[11], (DK,), jnp.float32), 0.1, 1.9)
    w_out = bell_draw(key_of[12], (HW, D), HW ** -0.5, 0.125, ((0, 4), (1, 8)))
    mixer_gain = jnp.clip(1.0 + 0.18 * jax.random.normal(key_of[13], (D,), jnp.float32), 0.099609375, 1.8984375).astype(jnp.bfloat16)
    w_gate = bell_draw(key_of[14], (D, FF), D ** -0.5, 0.09375, ((0, 8), (1, 4)))
    w_up = bell_draw(key_of[15], (D, FF), D ** -0.5, 0.09375, ((0, 8), (1, 4)))
    w_down = bell_draw(key_of[16], (FF, D), FF ** -0.5, 0.0546875, ((0, 4), (1, 8)))
    return dict(layer_input=layer_input, seq_lengths=seq_lengths, delta_state=delta_state, attn_gain=attn_gain, w_query=w_query, w_key=w_key, w_value=w_value, w_outgate=w_outgate, w_write=w_write, w_forget=w_forget, forget_rate=forget_rate, head_gain=head_gain, w_out=w_out, mixer_gain=mixer_gain, w_gate=w_gate, w_up=w_up, w_down=w_down)


EPS = 1e-06

def unit_norm(vectors):
    return vectors * lax.rsqrt(lax.optimization_barrier(jnp.sum(vectors * vectors, axis=-1, keepdims=True)) + EPS)

def run_delta(carried, query_unit, key_unit, value_act, write_rate, log_keep, live):
    readings = []
    for position in range(query_unit.shape[1]):
        active = live[:, position][:, None]
        beta = write_rate[:, position] * active
        keep = jnp.exp(log_keep[:, position] * active)
        key_now = key_unit[:, position]
        recalled = jnp.einsum('shk,shkv->shv', key_now, carried, precision=lax.Precision.HIGHEST)
        update = beta[:, :, None] * (value_act[:, position] - keep[:, :, None] * recalled)
        carried = keep[:, :, None, None] * carried + key_now[:, :, :, None] * update[:, :, None, :]
        reading = jnp.einsum('shk,shkv->shv', query_unit[:, position], carried, precision=lax.Precision.HIGHEST)
        readings.append(reading * active[:, :, None])
    return (carried, jnp.stack(readings, axis=1))

def reference(layer_input, seq_lengths, delta_state, attn_gain, w_query, w_key, w_value, w_outgate, w_write, w_forget, forget_rate, head_gain, w_out, mixer_gain, w_gate, w_up, w_down):
    rows_wide = layer_input.astype(jnp.float32)
    first_scale = lax.rsqrt(lax.optimization_barrier(jnp.mean(rows_wide * rows_wide, axis=1, keepdims=True)) + EPS)
    normed_in = (rows_wide * attn_gain.astype(jnp.float32)).astype(jnp.bfloat16)

    def project(weight):
        return first_scale * jnp.dot(normed_in, weight, preferred_element_type=jnp.float32)

    def split_heads(block):
        return block.reshape(SEQS, NEW, H, DK)
    query_unit = unit_norm(jax.nn.silu(split_heads(project(w_query)))) * DK ** (-0.5)
    key_unit = unit_norm(jax.nn.silu(split_heads(project(w_key))))
    value_act = jax.nn.silu(split_heads(project(w_value)))
    outgate = split_heads(project(w_outgate))
    write_rate = jax.nn.sigmoid(project(w_write).reshape(SEQS, NEW, H))
    log_keep = -forget_rate * jax.nn.softplus(project(w_forget).reshape(SEQS, NEW, H))
    positions = jnp.arange(NEW, dtype=jnp.int32)
    live = (positions[None, :] < seq_lengths[:, None]).astype(jnp.float32)
    carried, readings = run_delta(delta_state, query_unit, key_unit, value_act, write_rate, log_keep, live)
    normed = readings * lax.rsqrt(lax.optimization_barrier(jnp.mean(readings * readings, axis=-1, keepdims=True)) + EPS)
    normed = normed * head_gain * jax.nn.silu(outgate)
    mixed = normed.reshape(ROWS, HW).astype(jnp.bfloat16)
    grouped = mixed.reshape(ROWS, N_TP, HW // N_TP).astype(jnp.float32)
    out_groups = w_out.reshape(N_TP, HW // N_TP, D).astype(jnp.float32)
    group_terms = jnp.einsum('rgc,gcd->grd', grouped, out_groups)
    attended = lax.optimization_barrier(jnp.sum(group_terms.astype(jnp.bfloat16).astype(jnp.float32), axis=0))
    hidden_state = (rows_wide + attended).astype(jnp.bfloat16)
    hidden_wide = hidden_state.astype(jnp.float32)
    mixer_scale = lax.rsqrt(lax.optimization_barrier(jnp.mean(hidden_wide * hidden_wide, axis=1, keepdims=True)) + EPS)
    normed_mid = (hidden_wide * mixer_gain.astype(jnp.float32)).astype(jnp.bfloat16)
    gate_pre = mixer_scale * jnp.dot(normed_mid, w_gate, preferred_element_type=jnp.float32)
    up_pre = mixer_scale * jnp.dot(normed_mid, w_up, preferred_element_type=jnp.float32)
    activated = (jax.nn.silu(gate_pre) * up_pre).astype(jnp.bfloat16)
    mixer_out = jnp.dot(activated, w_down, preferred_element_type=jnp.float32)
    layer_output = (hidden_wide + mixer_out).astype(jnp.bfloat16)
    return (layer_output, carried)
```

```python
import functools

import jax
import jax.numpy as jnp
from jax import lax
from jax.experimental import pallas as pl
from jax.experimental.pallas import tpu as pltpu
from jax.sharding import PartitionSpec as P

MESH = pl.DeviceIdType.MESH
D = 4096
NEW = 4
EPS = 1e-06
LANES = 128
F32 = jnp.float32
BF16 = jnp.bfloat16


def grid_of(n_kv):
    nx = 1
    while nx * nx * 8 <= n_kv:
        nx *= 2
    return n_kv // nx, nx


def groups_of(width, count):
    units = width // LANES
    count = min(count, units)
    sizes = [units // count + (1 if i < units % count else 0) for i in range(count)]
    spans, at = [], 0
    for size in sizes:
        spans.append((at * LANES, size * LANES))
        at += size
    return spans


class Net:
    def __init__(self, n_kv, n_tp, send_sem, recv_sem):
        self.n_kv, self.n_tp = n_kv, n_tp
        self.nz, self.nx = grid_of(n_kv)
        self.kv, self.tp = lax.axis_index("kv"), lax.axis_index("tp")
        self.z, self.x = self.kv // self.nx, self.kv % self.nx
        self.send_sem, self.recv_sem = send_sem, recv_sem
        self.started = []

    def tp_peer(self, d):
        return (self.tp + d) % self.n_tp

    def kv_peer(self, d):
        return (self.kv + d) % self.n_kv

    def z_peer(self, d):
        return (self.z + d) % self.nz

    def x_peer(self, d):
        return (self.x + d) % self.nx

    def barrier(self):
        sem = pltpu.get_barrier_semaphore()
        for d in range(1, self.n_tp):
            pl.semaphore_signal(
                sem, inc=1, device_id={"kv": self.kv, "tp": self.tp_peer(d)}, device_id_type=MESH
            )
        for d in range(1, self.n_kv):
            pl.semaphore_signal(
                sem, inc=1, device_id={"kv": self.kv_peer(d), "tp": self.tp}, device_id_type=MESH
            )
        pl.semaphore_wait(sem, self.n_tp + self.n_kv - 2)

    def send(self, src, dst, kv, tp):
        at = len(self.started)
        copy = pltpu.make_async_remote_copy(
            src_ref=src,
            dst_ref=dst,
            send_sem=self.send_sem.at[at],
            recv_sem=self.recv_sem.at[at],
            device_id={"kv": kv, "tp": tp},
            device_id_type=MESH,
        )
        copy.start()
        self.started.append(copy)
        return copy

    def drain(self):
        for copy in self.started:
            copy.wait_send()


def arrive(copies):
    for copy in copies:
        copy.wait_recv()


def gather_tp(net, src, dst):
    return [net.send(src, dst.at[net.tp], net.kv, net.tp_peer(d)) for d in range(1, net.n_tp)]


def scatter_tp(net, src, dst):
    return [
        net.send(src.at[net.tp_peer(d)], dst.at[d - 1], net.kv, net.tp_peer(d))
        for d in range(1, net.n_tp)
    ]


def gather_kv(net, src, dst):
    return [net.send(src, dst.at[net.kv], net.kv_peer(d), net.tp) for d in range(1, net.n_kv)]


def scatter_kv(net, src, dst):
    return [
        net.send(src.at[net.kv_peer(d)], dst.at[d - 1], net.kv_peer(d), net.tp)
        for d in range(1, net.n_kv)
    ]


def scatter_x(net, parts, got, cols):
    return [
        net.send(
            parts.at[net.x_peer(d), :, cols],
            got.at[d - 1, :, cols],
            net.z * net.nx + net.x_peer(d),
            net.tp,
        )
        for d in range(1, net.nx)
    ]


def scatter_z(net, parts, got, cols):
    return [
        net.send(
            parts.at[net.z_peer(d), :, cols],
            got.at[d - 1, :, cols],
            net.z_peer(d) * net.nx + net.x,
            net.tp,
        )
        for d in range(1, net.nz)
    ]


def store_parts(net, parts, product, cols):
    own = product.shape[0] // net.n_kv
    for block in range(net.n_kv):
        z, x = block // net.nx, block % net.nx
        parts[x, z * own : (z + 1) * own, cols] = product[block * own : (block + 1) * own].astype(
            BF16
        )


def fold_x(net, parts, got, folded, cols):
    total = parts[net.x, :, cols].astype(F32)
    for d in range(1, net.nx):
        total = total + got[d - 1, :, cols].astype(F32)
    folded[:, :, cols] = total.astype(BF16).reshape(net.nz, -1, total.shape[1])


def fold_z(net, folded, got, cols):
    total = folded[net.z, :, cols].astype(F32)
    for d in range(1, net.nz):
        total = total + got[d - 1, :, cols].astype(F32)
    return total


def project_kernel(
    n_kv,
    n_tp,
    x_ref,
    gain_ref,
    rate_ref,
    wq_hbm,
    wk_hbm,
    wv_hbm,
    wo_hbm,
    out_ref,
    aux_out_ref,
    weights,
    x_all,
    aux,
    aux_got,
    parts,
    x_got,
    folded,
    z_got,
    load_sem,
    send_sem,
    recv_sem,
):
    net = Net(n_kv, n_tp, send_sem, recv_sem)
    loads = []
    for i, source in enumerate((wq_hbm, wk_hbm, wv_hbm, wo_hbm)):
        copy = pltpu.make_async_copy(source, weights.at[i], load_sem.at[i])
        copy.start()
        loads.append(copy)
    net.barrier()
    incoming = gather_tp(net, x_ref, x_all)
    x_all[net.tp] = x_ref[...]
    arrive(incoming)
    wide = x_all[...].reshape(-1, x_ref.shape[1]).astype(F32)
    squares = jnp.sum(wide * wide, axis=1, keepdims=True)
    normed = (wide * gain_ref[net.kv]).astype(BF16)
    rates = jnp.dot(normed, rate_ref[...], preferred_element_type=F32)
    lane = lax.broadcasted_iota(jnp.int32, rates.shape, 1)
    aux[...] = jnp.where(lane == LANES - 1, squares, rates).reshape(aux.shape)
    aux_in = scatter_kv(net, aux, aux_got)
    width = weights.shape[2]
    crossing = []
    for i in range(4):
        cols = pl.ds(i * width, width)
        loads[i].wait()
        product = jnp.dot(normed, weights[i], preferred_element_type=F32)
        store_parts(net, parts, product, cols)
        crossing.append(scatter_x(net, parts, x_got, cols))
    climbing = []
    for i in range(4):
        cols = pl.ds(i * width, width)
        arrive(crossing[i])
        fold_x(net, parts, x_got, folded, cols)
        climbing.append(scatter_z(net, folded, z_got, cols))
    arrive(aux_in)
    aux_out_ref[...] = aux[net.kv] + jnp.sum(aux_got[...], axis=0)
    for i in range(4):
        cols = pl.ds(i * width, width)
        arrive(climbing[i])
        out_ref[:, cols] = fold_z(net, folded, z_got, cols)
    net.drain()


def mixer_kernel(
    n_kv,
    n_tp,
    n_groups,
    mixed_ref,
    x_ref,
    gain_ref,
    w_out_hbm,
    w_gate_hbm,
    w_up_hbm,
    w_down_hbm,
    out_ref,
    w_out,
    w_gate,
    w_up,
    w_down,
    mixed_all,
    out_parts,
    out_got,
    hidden_all,
    aux,
    aux_got,
    parts,
    x_got,
    folded,
    z_got,
    act,
    down_parts,
    down_got,
    load_sem,
    send_sem,
    recv_sem,
):
    net = Net(n_kv, n_tp, send_sem, recv_sem)
    loads = []
    pairs = ((w_out_hbm, w_out), (w_gate_hbm, w_gate), (w_up_hbm, w_up), (w_down_hbm, w_down))
    for i, (source, target) in enumerate(pairs):
        copy = pltpu.make_async_copy(source, target, load_sem.at[i])
        copy.start()
        loads.append(copy)
    net.barrier()
    incoming = gather_kv(net, mixed_ref, mixed_all)
    mixed_all[net.kv] = mixed_ref[...]
    arrive(incoming)
    loads[0].wait()
    terms = jnp.dot(
        mixed_all[...].reshape(-1, mixed_ref.shape[1]), w_out[...], preferred_element_type=F32
    )
    out_parts[...] = terms.astype(BF16).reshape(out_parts.shape)
    arrive(scatter_tp(net, out_parts, out_got))
    attended = out_parts[net.tp].astype(F32)
    for d in range(1, n_tp):
        attended = attended + out_got[d - 1].astype(F32)
    hidden = (x_ref[...].astype(F32) + attended).astype(BF16)
    hidden_all[net.tp] = hidden
    arrive(gather_tp(net, hidden_all.at[net.tp], hidden_all))
    wide = hidden_all[...].reshape(-1, x_ref.shape[1]).astype(F32)
    squares = jnp.sum(wide * wide, axis=1, keepdims=True)
    normed = (wide * gain_ref[net.kv]).astype(BF16)
    aux[...] = jnp.broadcast_to(squares, (squares.shape[0], LANES)).reshape(aux.shape)
    aux_in = scatter_kv(net, aux, aux_got)
    spans = groups_of(w_gate.shape[1], n_groups)
    count = len(spans)
    crossing, climbing, rising, spreading = [], [], [], []
    loads[1].wait()
    loads[2].wait()
    for at, size in spans:
        store_parts(
            net,
            parts,
            jnp.dot(normed, w_gate[:, pl.ds(at, size)], preferred_element_type=F32),
            pl.ds(2 * at, size),
        )
        store_parts(
            net,
            parts,
            jnp.dot(normed, w_up[:, pl.ds(at, size)], preferred_element_type=F32),
            pl.ds(2 * at + size, size),
        )
        crossing.append(scatter_x(net, parts, x_got, pl.ds(2 * at, 2 * size)))
    arrive(aux_in)
    total = aux[net.kv]
    for d in range(1, n_kv):
        total = total + aux_got[d - 1]
    scale = lax.rsqrt(total[:, :1] / D + EPS)
    loads[3].wait()
    down = None
    for step in range(count + 3):
        if step < count:
            at, size = spans[step]
            cols = pl.ds(2 * at, 2 * size)
            arrive(crossing[step])
            fold_x(net, parts, x_got, folded, cols)
            climbing.append(scatter_z(net, folded, z_got, cols))
        if 0 <= step - 1 < count:
            at, size = spans[step - 1]
            arrive(climbing[step - 1])
            gate = fold_z(net, folded, z_got, pl.ds(2 * at, size)) * scale
            up = fold_z(net, folded, z_got, pl.ds(2 * at + size, size)) * scale
            act[net.z, net.x, :, pl.ds(at, size)] = (jax.nn.silu(gate) * up).astype(BF16)
            block = act.at[net.z, net.x, :, pl.ds(at, size)]
            rising.append(
                [
                    net.send(block, block, net.z_peer(d) * net.nx + net.x, net.tp)
                    for d in range(1, net.nz)
                ]
            )
        if 0 <= step - 2 < count:
            at, size = spans[step - 2]
            arrive(rising[step - 2])
            block = act.at[:, net.x, :, pl.ds(at, size)]
            spreading.append(
                [
                    net.send(block, block, net.z * net.nx + net.x_peer(d), net.tp)
                    for d in range(1, net.nx)
                ]
            )
        if 0 <= step - 3 < count:
            at, size = spans[step - 3]
            arrive(spreading[step - 3])
            block = act[:, :, :, pl.ds(at, size)].reshape(-1, size)
            term = jnp.dot(block, w_down[pl.ds(at, size), :], preferred_element_type=F32)
            down = term if down is None else down + term
    down_parts[...] = down.astype(BF16).reshape(down_parts.shape)
    arrive(scatter_tp(net, down_parts, down_got))
    result = down_parts[net.tp].astype(F32)
    for d in range(1, n_tp):
        result = result + down_got[d - 1].astype(F32)
    out_ref[...] = (hidden_all[net.tp].astype(F32) + result).astype(BF16)
    net.drain()


def vmem():
    return pl.BlockSpec(memory_space=pltpu.VMEM)


def hbm():
    return pl.BlockSpec(memory_space=pl.ANY)


def params(collective_id):
    return pltpu.CompilerParams(
        collective_id=collective_id, has_side_effects=True, vmem_limit_bytes=56 * 1024 * 1024
    )


def unit_norm(vectors):
    return vectors * lax.rsqrt(jnp.sum(vectors * vectors, axis=-1, keepdims=True) + EPS)


def run_delta(carried, query_unit, key_unit, value_act, write_rate, log_keep, live):
    readings = []
    for position in range(query_unit.shape[1]):
        active = live[:, position][:, None]
        beta = write_rate[:, position] * active
        keep = jnp.exp(log_keep[:, position] * active)
        key_now = key_unit[:, position]
        recalled = jnp.einsum("shk,shkv->shv", key_now, carried, precision=lax.Precision.HIGHEST)
        update = beta[:, :, None] * (value_act[:, position] - keep[:, :, None] * recalled)
        carried = keep[:, :, None, None] * carried + key_now[:, :, :, None] * update[:, :, None, :]
        reading = jnp.einsum(
            "shk,shkv->shv", query_unit[:, position], carried, precision=lax.Precision.HIGHEST
        )
        readings.append(reading * active[:, :, None])
    return (carried, jnp.stack(readings, axis=1))


def local(
    n_kv,
    n_tp,
    layer_input,
    seq_lengths,
    delta_state,
    attn_gain,
    w_query,
    w_key,
    w_value,
    w_outgate,
    w_write,
    w_forget,
    forget_rate,
    head_gain,
    w_out,
    mixer_gain,
    w_gate,
    w_up,
    w_down,
):
    tp_rows, features = layer_input.shape
    rows = tp_rows * n_tp
    own = rows // n_kv
    nz, nx = grid_of(n_kv)
    head_cols = w_query.shape[1]
    seqs_here = seq_lengths.shape[0]
    heads_here = forget_rate.shape[0]
    head_size = head_gain.shape[0]
    rate_weight = jnp.pad(
        jnp.concatenate([w_write, w_forget], axis=1), ((0, 0), (0, LANES - 2 * heads_here))
    )
    copies = (n_tp - 1) + (n_kv - 1) + 4 * (nx - 1 + nz - 1)
    sums, aux = pl.pallas_call(
        functools.partial(project_kernel, n_kv, n_tp),
        out_shape=(
            jax.ShapeDtypeStruct((own, 4 * head_cols), F32),
            jax.ShapeDtypeStruct((own, LANES), F32),
        ),
        in_specs=[vmem()] * 3 + [hbm()] * 4,
        out_specs=(vmem(), vmem()),
        scratch_shapes=[
            pltpu.VMEM((4, features, head_cols), BF16),
            pltpu.VMEM((n_tp, tp_rows, features), BF16),
            pltpu.VMEM((n_kv, own, LANES), F32),
            pltpu.VMEM((n_kv - 1, own, LANES), F32),
            pltpu.VMEM((nx, nz * own, 4 * head_cols), BF16),
            pltpu.VMEM((nx - 1, nz * own, 4 * head_cols), BF16),
            pltpu.VMEM((nz, own, 4 * head_cols), BF16),
            pltpu.VMEM((nz - 1, own, 4 * head_cols), BF16),
            pltpu.SemaphoreType.DMA((4,)),
            pltpu.SemaphoreType.DMA((copies,)),
            pltpu.SemaphoreType.DMA((copies,)),
        ],
        compiler_params=params(0),
    )(
        layer_input,
        attn_gain.astype(F32).reshape(n_kv, 1, features),
        rate_weight,
        w_query,
        w_key,
        w_value,
        w_outgate,
    )
    row_scale = lax.rsqrt(aux[:, LANES - 1 :] / D + EPS)

    def split_heads(at):
        block = sums[:, at * head_cols : (at + 1) * head_cols]
        return (block * row_scale).reshape(seqs_here, NEW, heads_here, head_size)

    query_unit = unit_norm(jax.nn.silu(split_heads(0))) * head_size ** (-0.5)
    key_unit = unit_norm(jax.nn.silu(split_heads(1)))
    value_act = jax.nn.silu(split_heads(2))
    outgate = split_heads(3)
    rate_rows = (aux[:, : 2 * heads_here] * row_scale).reshape(seqs_here, NEW, 2 * heads_here)
    write_rate = jax.nn.sigmoid(rate_rows[:, :, :heads_here])
    log_keep = -forget_rate * jax.nn.softplus(rate_rows[:, :, heads_here:])
    positions = jnp.arange(NEW, dtype=jnp.int32)
    live = (positions[None, :] < seq_lengths[:, None]).astype(F32)
    carried, readings = run_delta(
        delta_state, query_unit, key_unit, value_act, write_rate, log_keep, live
    )
    normed = readings * lax.rsqrt(jnp.mean(readings * readings, axis=-1, keepdims=True) + EPS)
    normed = normed * head_gain * jax.nn.silu(outgate)
    mixed = normed.reshape(own, heads_here * head_size).astype(BF16)

    hidden_cols = w_gate.shape[1]
    n_groups = 6
    groups = len(groups_of(hidden_cols, n_groups))
    copies = 3 * (n_tp - 1) + 2 * (n_kv - 1) + 2 * groups * (nx - 1 + nz - 1)
    layer_output = pl.pallas_call(
        functools.partial(mixer_kernel, n_kv, n_tp, n_groups),
        out_shape=jax.ShapeDtypeStruct((tp_rows, features), BF16),
        in_specs=[vmem()] * 3 + [hbm()] * 4,
        out_specs=vmem(),
        scratch_shapes=[
            pltpu.VMEM(w_out.shape, BF16),
            pltpu.VMEM(w_gate.shape, BF16),
            pltpu.VMEM(w_up.shape, BF16),
            pltpu.VMEM(w_down.shape, BF16),
            pltpu.VMEM((n_kv, own, head_cols), BF16),
            pltpu.VMEM((n_tp, tp_rows, features), BF16),
            pltpu.VMEM((n_tp - 1, tp_rows, features), BF16),
            pltpu.VMEM((n_tp, tp_rows, features), BF16),
            pltpu.VMEM((n_kv, own, LANES), F32),
            pltpu.VMEM((n_kv - 1, own, LANES), F32),
            pltpu.VMEM((nx, nz * own, 2 * hidden_cols), BF16),
            pltpu.VMEM((nx - 1, nz * own, 2 * hidden_cols), BF16),
            pltpu.VMEM((nz, own, 2 * hidden_cols), BF16),
            pltpu.VMEM((nz - 1, own, 2 * hidden_cols), BF16),
            pltpu.VMEM((nz, nx, own, hidden_cols), BF16),
            pltpu.VMEM((n_tp, tp_rows, features), BF16),
            pltpu.VMEM((n_tp - 1, tp_rows, features), BF16),
            pltpu.SemaphoreType.DMA((4,)),
            pltpu.SemaphoreType.DMA((copies,)),
            pltpu.SemaphoreType.DMA((copies,)),
        ],
        compiler_params=params(1),
    )(
        mixed,
        layer_input,
        mixer_gain.astype(F32).reshape(n_kv, 1, features),
        w_out,
        w_gate,
        w_up,
        w_down,
    )
    return (layer_output, carried)


def solution(mesh):
    in_specs = (
        P("tp", "kv"),
        P("kv"),
        P("kv", "tp", None, None),
        P(),
        P("kv", "tp"),
        P("kv", "tp"),
        P("kv", "tp"),
        P("kv", "tp"),
        P("kv", "tp"),
        P("kv", "tp"),
        P("tp"),
        P(),
        P("tp", "kv"),
        P(),
        P("kv", "tp"),
        P("kv", "tp"),
        P("tp", "kv"),
    )
    out_specs = (P("tp", "kv"), P("kv", "tp", None, None))
    body = functools.partial(local, mesh.shape["kv"], mesh.shape["tp"])
    return jax.shard_map(body, mesh=mesh, in_specs=in_specs, out_specs=out_specs, check_vma=False)
```

```python
import functools

import jax
import jax.numpy as jnp
from jax import lax
from jax.experimental import pallas as pl
from jax.experimental.pallas import tpu as pltpu
from jax.sharding import PartitionSpec as P

MESH = pl.DeviceIdType.MESH
D = 4096
NEW = 4
EPS = 1e-06
LANES = 128
F32 = jnp.float32
BF16 = jnp.bfloat16


def grid_of(n_kv):
    nx = 1
    while nx * nx * 8 <= n_kv:
        nx *= 2
    return n_kv // nx, nx


def groups_of(width, count):
    units = width // LANES
    count = min(count, units)
    sizes = [units // count + (1 if i < units % count else 0) for i in range(count)]
    spans, at = [], 0
    for size in sizes:
        spans.append((at * LANES, size * LANES))
        at += size
    return spans


class Net:
    def __init__(self, n_kv, n_tp, send_sem, recv_sem):
        self.n_kv, self.n_tp = n_kv, n_tp
        self.nz, self.nx = grid_of(n_kv)
        self.kv, self.tp = lax.axis_index("kv"), lax.axis_index("tp")
        self.z, self.x = self.kv // self.nx, self.kv % self.nx
        self.send_sem, self.recv_sem = send_sem, recv_sem
        self.started = []

    def tp_peer(self, d):
        return (self.tp + d) % self.n_tp

    def kv_peer(self, d):
        return (self.kv + d) % self.n_kv

    def z_peer(self, d):
        return (self.z + d) % self.nz

    def x_peer(self, d):
        return (self.x + d) % self.nx

    def barrier(self):
        sem = pltpu.get_barrier_semaphore()
        for d in range(1, self.n_tp):
            pl.semaphore_signal(
                sem, inc=1, device_id={"kv": self.kv, "tp": self.tp_peer(d)}, device_id_type=MESH
            )
        for d in range(1, self.n_kv):
            pl.semaphore_signal(
                sem, inc=1, device_id={"kv": self.kv_peer(d), "tp": self.tp}, device_id_type=MESH
            )
        pl.semaphore_wait(sem, self.n_tp + self.n_kv - 2)

    def send(self, src, dst, kv, tp):
        at = len(self.started)
        copy = pltpu.make_async_remote_copy(
            src_ref=src,
            dst_ref=dst,
            send_sem=self.send_sem.at[at],
            recv_sem=self.recv_sem.at[at],
            device_id={"kv": kv, "tp": tp},
            device_id_type=MESH,
        )
        copy.start()
        self.started.append(copy)
        return copy

    def drain(self):
        for copy in self.started:
            copy.wait_send()


def arrive(copies):
    for copy in copies:
        copy.wait_recv()


def gather_tp(net, src, dst):
    return [net.send(src, dst.at[net.tp], net.kv, net.tp_peer(d)) for d in range(1, net.n_tp)]


def scatter_tp(net, src, dst):
    return [
        net.send(src.at[net.tp_peer(d)], dst.at[d - 1], net.kv, net.tp_peer(d))
        for d in range(1, net.n_tp)
    ]


def gather_kv(net, src, dst):
    return [net.send(src, dst.at[net.kv], net.kv_peer(d), net.tp) for d in range(1, net.n_kv)]


def scatter_kv(net, src, dst):
    return [
        net.send(src.at[net.kv_peer(d)], dst.at[d - 1], net.kv_peer(d), net.tp)
        for d in range(1, net.n_kv)
    ]


def scatter_x(net, parts, got, cols):
    return [
        net.send(
            parts.at[net.x_peer(d), :, cols],
            got.at[d - 1, :, cols],
            net.z * net.nx + net.x_peer(d),
            net.tp,
        )
        for d in range(1, net.nx)
    ]


def scatter_z(net, parts, got, cols):
    return [
        net.send(
            parts.at[net.z_peer(d), :, cols],
            got.at[d - 1, :, cols],
            net.z_peer(d) * net.nx + net.x,
            net.tp,
        )
        for d in range(1, net.nz)
    ]


def store_parts(net, parts, product, cols):
    own = product.shape[0] // net.n_kv
    for block in range(net.n_kv):
        z, x = block // net.nx, block % net.nx
        parts[x, z * own : (z + 1) * own, cols] = product[block * own : (block + 1) * own].astype(
            BF16
        )


def fold_x(net, parts, got, folded, cols):
    total = parts[net.x, :, cols].astype(F32)
    for d in range(1, net.nx):
        total = total + got[d - 1, :, cols].astype(F32)
    folded[:, :, cols] = total.astype(BF16).reshape(net.nz, -1, total.shape[1])


def fold_z(net, folded, got, cols):
    total = folded[net.z, :, cols].astype(F32)
    for d in range(1, net.nz):
        total = total + got[d - 1, :, cols].astype(F32)
    return total


def split(value):
    high = value.astype(BF16).astype(F32)
    return high, value - high


def unit_norm(vectors):
    return vectors * lax.rsqrt(jnp.sum(vectors * vectors, axis=-1, keepdims=True) + EPS)


def softplus(value):
    return jnp.maximum(value, 0.0) + jnp.log1p(jnp.exp(-jnp.abs(value)))


def layer_kernel(
    n_kv,
    n_tp,
    n_groups,
    x_ref,
    attn_gain_ref,
    rate_ref,
    lengths_ref,
    forget_ref,
    head_gain_ref,
    mixer_gain_ref,
    wq_hbm,
    wk_hbm,
    wv_hbm,
    wo_hbm,
    w_out_hbm,
    w_gate_hbm,
    w_up_hbm,
    w_down_hbm,
    state_hbm,
    out_ref,
    state_out,
    aux1,
    aux1_got,
    parts1,
    x1_got,
    folded1,
    z1_got,
    weights,
    x_all,
    state,
    state_hi,
    state_lo,
    pre,
    aux_sum,
    lhs,
    recalled,
    left,
    right,
    keep_all,
    mixed_rows,
    w_out,
    w_gate,
    w_up,
    w_down,
    mixed_all,
    out_parts,
    out_got,
    hidden_all,
    aux,
    aux_got,
    parts,
    x_got,
    folded,
    z_got,
    act,
    down_parts,
    down_got,
    load_sem,
    send_sem,
    recv_sem,
):
    net = Net(n_kv, n_tp, send_sem, recv_sem)
    loads = []
    pairs = (
        (wq_hbm, weights.at[0]),
        (wk_hbm, weights.at[1]),
        (wv_hbm, weights.at[2]),
        (wo_hbm, weights.at[3]),
        (w_out_hbm, w_out),
        (w_gate_hbm, w_gate),
        (w_up_hbm, w_up),
        (w_down_hbm, w_down),
        (state_hbm, state),
    )
    for i in (0, 1, 2, 3, 8, 4, 5, 6, 7):
        pltpu.make_async_copy(*pairs[i], load_sem.at[i]).start()
    loads = [pltpu.make_async_copy(*pair, load_sem.at[i]) for i, pair in enumerate(pairs)]
    net.barrier()
    incoming = gather_tp(net, x_ref, x_all)
    x_all[net.tp] = x_ref[...]
    arrive(incoming)
    wide = x_all[...].reshape(-1, x_ref.shape[1]).astype(F32)
    squares = jnp.sum(wide * wide, axis=1, keepdims=True)
    normed = (wide * attn_gain_ref[net.kv]).astype(BF16)
    rates = jnp.dot(normed, rate_ref[...], preferred_element_type=F32)
    lane = lax.broadcasted_iota(jnp.int32, rates.shape, 1)
    aux1[...] = jnp.where(lane == LANES - 1, squares, rates).reshape(aux1.shape)
    aux_in = scatter_kv(net, aux1, aux1_got)
    width = weights.shape[2]
    crossing = []
    for i in range(4):
        cols = pl.ds(i * width, width)
        loads[i].wait()
        product = jnp.dot(normed, weights[i], preferred_element_type=F32)
        store_parts(net, parts1, product, cols)
        crossing.append(scatter_x(net, parts1, x1_got, cols))
    climbing = []
    for i in range(4):
        cols = pl.ds(i * width, width)
        arrive(crossing[i])
        fold_x(net, parts1, x1_got, folded1, cols)
        climbing.append(scatter_z(net, folded1, z1_got, cols))

    seqs, heads, size = state.shape[0], state.shape[1], state.shape[2]
    pieces = seqs * heads
    arrive(aux_in)
    aux_sum[...] = aux1[net.kv] + jnp.sum(aux1_got[...], axis=0)
    loads[8].wait()
    for h in range(heads):
        for s in range(seqs):
            high = state[s, h].astype(BF16)
            state_hi[h * seqs + s] = high
            state_lo[h * seqs + s] = (state[s, h] - high.astype(F32)).astype(BF16)
    for i in range(4):
        cols = pl.ds(i * width, width)
        arrive(climbing[i])
        total = fold_z(net, folded1, z1_got, cols)
        for h in range(heads):
            pre[i * heads + h] = total[:, h * size : (h + 1) * size]

    def stacked(at, t):
        return jnp.concatenate(
            [
                pre[at * heads + h, pl.ds(t, seqs, stride=NEW), :]
                for h in range(heads)
            ],
            axis=0,
        )

    def tall(parts_of):
        return jnp.concatenate(parts_of, axis=0)

    keys, values, queries, writes, keeps, lives, scales = [], [], [], [], [], [], []
    for t in range(NEW):
        sums = aux_sum[pl.ds(t, seqs, stride=NEW), :]
        row_scale = lax.rsqrt(sums[:, LANES - 1 :] / D + EPS)
        live_rows = (lengths_ref[...] > t).astype(F32)
        scale = tall([row_scale] * heads)
        live = tall([live_rows] * heads)
        write = tall([sums[:, h : h + 1] for h in range(heads)]) * scale
        forget = tall([sums[:, heads + h : heads + h + 1] for h in range(heads)]) * scale
        rate = tall([jnp.full((seqs, 1), forget_ref[h], F32) for h in range(heads)])
        scales.append(scale)
        lives.append(live)
        writes.append(jax.nn.sigmoid(write) * live)
        keeps.append(jnp.exp(-rate * softplus(forget) * live))
        queries.append(unit_norm(jax.nn.silu(stacked(0, t) * scale)) * size ** (-0.5))
        keys.append(unit_norm(jax.nn.silu(stacked(1, t) * scale)))
        values.append(jax.nn.silu(stacked(2, t) * scale))
        k_high, k_low = split(keys[t])
        q_high, q_low = split(queries[t])
        for place, rows in enumerate((k_high, q_high, k_low, q_low)):
            lhs[pl.ds(place * NEW + t, pieces, stride=4 * NEW), :] = rows
    for i in range(pieces):
        block = lhs[i * 4 * NEW : (i + 1) * 4 * NEW, :].astype(BF16)
        product = jnp.dot(block, state_hi[i], preferred_element_type=F32)
        product = product + jnp.dot(block, state_lo[i], preferred_element_type=F32)
        recalled[i * 2 * NEW : (i + 1) * 2 * NEW, :] = product[: 2 * NEW] + product[2 * NEW :]
    ahead = jnp.ones((pieces, 1), F32)
    decay, updates = [], []
    for t in range(NEW):
        seen = ahead * recalled[pl.ds(t, pieces, stride=2 * NEW), :]
        for j in range(t):
            match = jnp.sum(keys[t] * keys[j], axis=-1, keepdims=True)
            seen = seen + (decay[j] * match) * updates[j]
        updates.append(writes[t] * (values[t] - keeps[t] * seen))
        ahead = ahead * keeps[t]
        decay = [item * keeps[t] for item in decay] + [jnp.ones((pieces, 1), F32)]
        reading = ahead * recalled[pl.ds(NEW + t, pieces, stride=2 * NEW), :]
        for j in range(t + 1):
            match = jnp.sum(queries[t] * keys[j], axis=-1, keepdims=True)
            reading = reading + (decay[j] * match) * updates[j]
        reading = reading * lives[t]
        normed_out = reading * lax.rsqrt(jnp.mean(reading * reading, axis=-1, keepdims=True) + EPS)
        normed_out = normed_out * head_gain_ref[...] * jax.nn.silu(stacked(3, t) * scales[t])
        for h in range(heads):
            mixed_rows[h, pl.ds(t, seqs, stride=NEW), :] = normed_out[h * seqs : (h + 1) * seqs]

    def update_state():
        keep_all[...] = jnp.broadcast_to(ahead, keep_all.shape)
        for j in range(NEW):
            k_high, k_low = split(decay[j] * keys[j])
            u_high, u_low = split(updates[j])
            for place, rows in enumerate((k_high, k_low, k_high, k_low)):
                left[pl.ds(place * NEW + j, pieces, stride=4 * NEW), :] = rows
            for place, rows in enumerate((u_high, u_high, u_low, u_low)):
                right[pl.ds(place * NEW + j, pieces, stride=4 * NEW), :] = rows
        for h in range(heads):
            for s in range(seqs):
                i = h * seqs + s
                rows = slice(i * 4 * NEW, (i + 1) * 4 * NEW)
                gained = lax.dot_general(
                    left[rows, :].astype(BF16),
                    right[rows, :].astype(BF16),
                    (((0,), (0,)), ((), ())),
                    preferred_element_type=F32,
                )
                state[s, h] = keep_all[i : i + 1, :] * state[s, h] + gained

    for h in range(heads):
        mixed_all[net.kv, :, pl.ds(h * size, size)] = mixed_rows[h].astype(BF16)
    incoming = gather_kv(net, mixed_all.at[net.kv], mixed_all)
    update_state()
    saving = pltpu.make_async_copy(state, state_out, load_sem.at[9])
    saving.start()
    arrive(incoming)
    loads[0 + 4].wait()
    terms = jnp.dot(
        mixed_all[...].reshape(-1, width), w_out[...], preferred_element_type=F32
    )
    out_parts[...] = terms.astype(BF16).reshape(out_parts.shape)
    arrive(scatter_tp(net, out_parts, out_got))
    attended = out_parts[net.tp].astype(F32)
    for d in range(1, n_tp):
        attended = attended + out_got[d - 1].astype(F32)
    hidden = (x_ref[...].astype(F32) + attended).astype(BF16)
    hidden_all[net.tp] = hidden
    arrive(gather_tp(net, hidden_all.at[net.tp], hidden_all))
    wide = hidden_all[...].reshape(-1, x_ref.shape[1]).astype(F32)
    squares = jnp.sum(wide * wide, axis=1, keepdims=True)
    normed = (wide * mixer_gain_ref[net.kv]).astype(BF16)
    aux[...] = jnp.broadcast_to(squares, (squares.shape[0], LANES)).reshape(aux.shape)
    aux_in = scatter_kv(net, aux, aux_got)
    spans = groups_of(w_gate.shape[1], n_groups)
    count = len(spans)
    crossing, climbing, rising, spreading = [], [], [], []
    loads[1 + 4].wait()
    loads[2 + 4].wait()
    for at, size in spans:
        store_parts(
            net,
            parts,
            jnp.dot(normed, w_gate[:, pl.ds(at, size)], preferred_element_type=F32),
            pl.ds(2 * at, size),
        )
        store_parts(
            net,
            parts,
            jnp.dot(normed, w_up[:, pl.ds(at, size)], preferred_element_type=F32),
            pl.ds(2 * at + size, size),
        )
        crossing.append(scatter_x(net, parts, x_got, pl.ds(2 * at, 2 * size)))
    arrive(aux_in)
    total = aux[net.kv]
    for d in range(1, n_kv):
        total = total + aux_got[d - 1]
    scale = lax.rsqrt(total[:, :1] / D + EPS)
    loads[3 + 4].wait()
    down = None
    for step in range(count + 3):
        if step < count:
            at, size = spans[step]
            cols = pl.ds(2 * at, 2 * size)
            arrive(crossing[step])
            fold_x(net, parts, x_got, folded, cols)
            climbing.append(scatter_z(net, folded, z_got, cols))
        if 0 <= step - 1 < count:
            at, size = spans[step - 1]
            arrive(climbing[step - 1])
            gate = fold_z(net, folded, z_got, pl.ds(2 * at, size)) * scale
            up = fold_z(net, folded, z_got, pl.ds(2 * at + size, size)) * scale
            act[net.z, net.x, :, pl.ds(at, size)] = (jax.nn.silu(gate) * up).astype(BF16)
            block = act.at[net.z, net.x, :, pl.ds(at, size)]
            rising.append(
                [
                    net.send(block, block, net.z_peer(d) * net.nx + net.x, net.tp)
                    for d in range(1, net.nz)
                ]
            )
        if 0 <= step - 2 < count:
            at, size = spans[step - 2]
            arrive(rising[step - 2])
            block = act.at[:, net.x, :, pl.ds(at, size)]
            spreading.append(
                [
                    net.send(block, block, net.z * net.nx + net.x_peer(d), net.tp)
                    for d in range(1, net.nx)
                ]
            )
        if 0 <= step - 3 < count:
            at, size = spans[step - 3]
            arrive(spreading[step - 3])
            block = act[:, :, :, pl.ds(at, size)].reshape(-1, size)
            term = jnp.dot(block, w_down[pl.ds(at, size), :], preferred_element_type=F32)
            down = term if down is None else down + term
    down_parts[...] = down.astype(BF16).reshape(down_parts.shape)
    arrive(scatter_tp(net, down_parts, down_got))
    result = down_parts[net.tp].astype(F32)
    for d in range(1, n_tp):
        result = result + down_got[d - 1].astype(F32)
    out_ref[...] = (hidden_all[net.tp].astype(F32) + result).astype(BF16)
    saving.wait()
    net.drain()


def vmem():
    return pl.BlockSpec(memory_space=pltpu.VMEM)


def hbm():
    return pl.BlockSpec(memory_space=pl.ANY)


def params(collective_id):
    return pltpu.CompilerParams(
        collective_id=collective_id, has_side_effects=True, vmem_limit_bytes=56 * 1024 * 1024
    )


def local(
    n_kv,
    n_tp,
    layer_input,
    seq_lengths,
    delta_state,
    attn_gain,
    w_query,
    w_key,
    w_value,
    w_outgate,
    w_write,
    w_forget,
    forget_rate,
    head_gain,
    w_out,
    mixer_gain,
    w_gate,
    w_up,
    w_down,
):
    tp_rows, features = layer_input.shape
    rows = tp_rows * n_tp
    own = rows // n_kv
    nz, nx = grid_of(n_kv)
    head_cols = w_query.shape[1]
    seqs, heads, size = delta_state.shape[:3]
    pieces = seqs * heads
    hidden_cols = w_gate.shape[1]
    rate_weight = jnp.pad(
        jnp.concatenate([w_write, w_forget], axis=1), ((0, 0), (0, LANES - 2 * heads))
    )
    n_groups = 6
    groups = len(groups_of(hidden_cols, n_groups))
    copies = 4 * (n_tp - 1) + 3 * (n_kv - 1) + (2 * groups + 4) * (nx - 1 + nz - 1)

    def reduce_buffers(cols):
        return [
            pltpu.VMEM((n_kv, own, LANES), F32),
            pltpu.VMEM((n_kv - 1, own, LANES), F32),
            pltpu.VMEM((nx, nz * own, cols), BF16),
            pltpu.VMEM((nx - 1, nz * own, cols), BF16),
            pltpu.VMEM((nz, own, cols), BF16),
            pltpu.VMEM((nz - 1, own, cols), BF16),
        ]

    row_block = pltpu.VMEM((n_tp, tp_rows, features), BF16)
    row_got = pltpu.VMEM((n_tp - 1, tp_rows, features), BF16)
    smem = pl.BlockSpec(memory_space=pltpu.SMEM)
    return pl.pallas_call(
        functools.partial(layer_kernel, n_kv, n_tp, n_groups),
        out_shape=(
            jax.ShapeDtypeStruct((tp_rows, features), BF16),
            jax.ShapeDtypeStruct(delta_state.shape, F32),
        ),
        in_specs=[vmem()] * 4 + [smem] + [vmem()] * 2 + [hbm()] * 9,
        out_specs=(vmem(), hbm()),
        scratch_shapes=reduce_buffers(4 * head_cols)
        + [
            pltpu.VMEM((4, features, head_cols), BF16),
            row_block,
            pltpu.VMEM(delta_state.shape, F32),
            pltpu.VMEM((pieces, size, size), BF16),
            pltpu.VMEM((pieces, size, size), BF16),
            pltpu.VMEM((4 * heads, own, size), F32),
            pltpu.VMEM((own, LANES), F32),
            pltpu.VMEM((pieces * 4 * NEW, size), F32),
            pltpu.VMEM((pieces * 2 * NEW, size), F32),
            pltpu.VMEM((pieces * 4 * NEW, size), F32),
            pltpu.VMEM((pieces * 4 * NEW, size), F32),
            pltpu.VMEM((pieces, LANES), F32),
            pltpu.VMEM((heads, own, size), F32),
            pltpu.VMEM(w_out.shape, BF16),
            pltpu.VMEM(w_gate.shape, BF16),
            pltpu.VMEM(w_up.shape, BF16),
            pltpu.VMEM(w_down.shape, BF16),
            pltpu.VMEM((n_kv, own, head_cols), BF16),
            row_block,
            row_got,
            row_block,
        ]
        + reduce_buffers(2 * hidden_cols)
        + [
            pltpu.VMEM((nz, nx, own, hidden_cols), BF16),
            row_block,
            row_got,
            pltpu.SemaphoreType.DMA((10,)),
            pltpu.SemaphoreType.DMA((copies,)),
            pltpu.SemaphoreType.DMA((copies,)),
        ],
        compiler_params=params(0),
    )(
        layer_input,
        attn_gain.astype(F32).reshape(n_kv, 1, features),
        rate_weight,
        seq_lengths.reshape(seqs, 1),
        forget_rate,
        head_gain.reshape(1, size),
        mixer_gain.astype(F32).reshape(n_kv, 1, features),
        w_query,
        w_key,
        w_value,
        w_outgate,
        w_out,
        w_gate,
        w_up,
        w_down,
        delta_state,
    )


def solution(mesh):
    in_specs = (
        P("tp", "kv"),
        P("kv"),
        P("kv", "tp", None, None),
        P(),
        P("kv", "tp"),
        P("kv", "tp"),
        P("kv", "tp"),
        P("kv", "tp"),
        P("kv", "tp"),
        P("kv", "tp"),
        P("tp"),
        P(),
        P("tp", "kv"),
        P(),
        P("kv", "tp"),
        P("kv", "tp"),
        P("tp", "kv"),
    )
    out_specs = (P("tp", "kv"), P("kv", "tp", None, None))
    body = functools.partial(local, mesh.shape["kv"], mesh.shape["tp"])
    return jax.shard_map(body, mesh=mesh, in_specs=in_specs, out_specs=out_specs, check_vma=False)
```
